32 devices in a mesh: sp: 8 (over z, x), dp: 4 (over y, core).
Axes of the slice: x: 2, y: 2, z: 4, core: 2. Of those that a mesh axis runs over, the one named last changes fastest.
Arguments:
- residual_in: bfloat16 [4, 1024, 2048], P('dp', 'sp'), may hold values from -6 to 6
- ssm_input: bfloat16 [4, 1024, 2048], P('dp', 'sp'), may hold values from -6 to 6
- state_b: bfloat16 [4, 1024, 2048], P('dp', 'sp'), may hold values from -6 to 6
- state_c: bfloat16 [4, 1024, 2048], P('dp', 'sp'), may hold values from -6 to 6
- step_raw: bfloat16 [4, 1024, 64], P('dp', 'sp'), may hold values from -4 to 3
- gate_input: bfloat16 [4, 1024, 2048], P('dp', 'sp'), may hold values from -6 to 6
- conv_x: float32 [7, 2048], P(None, 'sp'), may hold values from -2 to 2
- conv_b: float32 [7, 2048], P(None, 'sp'), may hold values from -2 to 2
- conv_c: float32 [7, 2048], P(None, 'sp'), may hold values from -2 to 2
- decay_rate: float32 [2, 32], P(None, 'sp'), may hold values from 0 to 1, as said below
- mix_gain: float32 [2048], replicated, may hold values from 0.1 to 1.9
- out_weight: bfloat16 [2048, 2048], P('dp'), may hold values from -0.125 to 0.125
- ffn_gain: float32 [2048], replicated, may hold values from 0.1 to 1.9
- routing: int32 [4, 1024, 4], P('dp', 'sp'), may hold values from 0 to 31, all different within a row; in each aligned block of 128 rows (0 to 127, 128 to 255, ..., all dimensions but the last counted through in order) at most 32 rows name the same one
- route_weight: float32 [4, 1024, 4], P('dp', 'sp'), may hold values from 0.1 to 0.6
- gate_w: bfloat16 [32, 2048, 1024], P(('sp', 'dp')), may hold values from -60 to 60
- up_w: bfloat16 [32, 2048, 1024], P(('sp', 'dp')), may hold values from -60 to 60
- down_w: bfloat16 [32, 1024, 2048], P(('sp', 'dp')), may hold values from -0.1875 to 0.1875
Outputs:
- block_out: bfloat16 [4, 1024, 2048], P('dp', 'sp')
The draws below stay inside these ranges and needn't reach their ends.
Inputs may be any that keep to these rules, and one draw needn't show every extreme that they name: `routing`: each row names 4 different experts; within the rows of one device no expert is named by more than 32 rows, a bound that some block reaches. `decay_rate`: Positive.
All inputs are finite; a program needn't handle non-finite values.
Results may differ from the reference program's by a relative error of at most 0.0082.
Values may be sent and summed in bfloat16 or wider, within the bound.
No kernel may reach another device: no remote copies, remote signals or barrier semaphores. Data moves between devices by JAX's collectives and lax.ppermute only.
A program may use at most 128 MiB of HBM per device.

```python
import math
import jax
import jax.numpy as jnp
import numpy as np
from jax import lax

D = 2048
HEADS = 32
HEAD_DIM = 64
GROUPS = 16
STATE = 128
CONV = 7
BLOCK = 128
NORM_GROUPS = 4
FF = 1024
TOPK = 4
TOK_DEV = 128
SEQ_LEN = 1024
SEQS = 4
EXPERTS = 32
CAP = 32


def draw_step_raw(key, part):
    noise_key, level_key = jax.random.split(key)
    noise = jnp.clip(jax.random.normal(noise_key, (SEQS, SEQ_LEN, 2 * HEADS), jnp.float32), -3.0, 3.0) * 0.5
    levels = jax.random.uniform(level_key, (SEQS, SEQ_LEN // TOK_DEV, 1, 2 * HEADS), jnp.float32, -2.0, 1.0)
    levels = jnp.broadcast_to(levels, (SEQS, SEQ_LEN // TOK_DEV, TOK_DEV, 2 * HEADS)).reshape(SEQS, SEQ_LEN, 2 * HEADS)
    return (noise + levels).astype(jnp.bfloat16)


def draw_decay_rate(key, part):
    pick_key, fast_key, slow_key = jax.random.split(key, 3)
    share = 0.5
    quick = jax.random.bernoulli(pick_key, share, (2, HEADS))
    fast_rate = jnp.exp(jax.random.uniform(fast_key, (2, HEADS), jnp.float32, math.log(0.02), math.log(0.2)))
    slow_rate = jnp.exp(jax.random.uniform(slow_key, (2, HEADS), jnp.float32, math.log(0.05), 0.0)) / SEQ_LEN
    return jnp.where(quick, fast_rate, slow_rate)


def expert_matrix(key):
    base_key, pick_key = jax.random.split(key)
    values = jnp.clip(jax.random.normal(base_key, (EXPERTS, D, FF), jnp.float32), -6.0, 6.0) * D ** (-0.5)
    values = values * 1.0
    return values


def draw_gate_w(key, part):
    return expert_matrix(jax.random.fold_in(key, 11)).astype(jnp.bfloat16)


def draw_up_w(key, part):
    return expert_matrix(jax.random.fold_in(key, 12)).astype(jnp.bfloat16)


def steps_of(rng, shape, pieces, least, top_value):
    level, own = 1.0, jax.random.fold_in(rng, 6)
    for axis_at, blocks in pieces:
        steps = jnp.exp(jax.random.uniform(jax.random.fold_in(own, axis_at), (blocks,), jnp.float32, least / len(pieces), top_value / len(pieces)))
        level = level * jnp.repeat(steps, shape[axis_at] // blocks).reshape([-1 if axis == axis_at else 1 for axis in range(len(shape))])
    return level


def shared_out(own_key, own, number, rows, amount, top, reach, slope):
    sequence = jax.random.permutation(own_key, amount)
    crowded, common = portions_of(amount, rows * top, reach, slope, True), portions_of(amount, rows * top, reach, slope, False)
    places = jnp.arange(amount)

    def named(tallies, turn):
        used = int((tallies > 0).sum())
        fixed = max(1, used // 4)
        moved = fixed + (places - fixed + turn * (used - fixed)) % max(1, amount - fixed)
        return jnp.zeros((amount,), jnp.int32).at[sequence[jnp.where(places < fixed, places, moved)]].set(jnp.asarray(tallies, jnp.int32))

    tallies = jnp.where(number % 4 == 0, named(crowded, number // 4), named(common, number - number // 4 - 1))
    mixed = jax.random.permutation(jax.random.fold_in(own, 3), amount)
    donor, receiver = mixed[0:amount // 2 * 2:2], mixed[1:amount // 2 * 2:2]
    room = jnp.minimum(tallies[donor] - 1, reach - tallies[receiver]) // 2
    room = jnp.where((donor == sequence[0]) | (receiver == sequence[0]) | (tallies[receiver] == 0), 0, jnp.maximum(room, 0))
    moved = jax.random.randint(jax.random.fold_in(own, 4), (amount // 2,), 0, 1 << 20) % (room + 1)
    tallies = tallies.at[donor].add(-moved).at[receiver].add(moved)
    items = jnp.searchsorted(jnp.cumsum(tallies), jnp.arange(rows * top), side="right").astype(jnp.int32)
    listing = items.reshape(top, rows).T
    listing = listing[jax.random.permutation(jax.random.fold_in(own, 1), rows)]
    turn = jax.random.randint(jax.random.fold_in(own, 2), (rows, 1), 0, top)
    return jnp.take_along_axis(listing, (jnp.arange(top)[None, :] + turn) % top, axis=1)


def portions_of(count, total, limit, skew, full):
    weights = [(1 << 20) // math.isqrt(rank ** skew) + 1 for rank in range(1, count + 1)]
    largest = limit if full else min(limit, max(-(-total // count), total * weights[0] // sum(weights)))
    least = 1 if total - largest >= count - 1 else 0
    holding, spare = [largest] + [least] * (count - 1), total - largest - least * (count - 1)
    while spare > 0:
        movable = [i for i in range(1, count) if holding[i] < largest] or [i for i in range(1, count) if holding[i] < limit]
        mass, budget = sum([weights[i] for i in movable]), spare
        for i in movable:
            addition = min(limit - holding[i], max(1, budget * weights[i] // mass), spare)
            holding[i] = holding[i] + addition
            spare = spare - addition
    return np.array(holding)


def gaussian(own_key, shape, width, limit, shards=(), kind=jnp.bfloat16):
    level = steps_of(own_key, shape, shards, -0.22, 0.18) if shards else 1.0
    values = jax.random.normal(own_key, shape, jnp.float32) * width * level
    return jnp.minimum(jnp.maximum(values, -limit), limit).astype(kind)


def setup_inputs(seed: int = 0) -> dict:
    key_of = jax.random.split(jax.random.key(seed), 19)
    residual_in = gaussian(key_of[0], (SEQS, SEQ_LEN, D), 1.0, 6.0, ((0, 4), (1, 8)))
    ssm_input = gaussian(key_of[1], (SEQS, SEQ_LEN, D), 1.0, 6.0, ((0, 4), (1, 8)))
    state_b = gaussian(key_of[2], (SEQS, SEQ_LEN, GROUPS * STATE), 1.0, 6.0, ((0, 4), (1, 8)))
    state_c = gaussian(key_of[3], (SEQS, SEQ_LEN, GROUPS * STATE), 1.0, 6.0, ((0, 4), (1, 8)))
    step_raw = draw_step_raw(jax.random.fold_in(key_of[18], 71), 0)
    gate_input = gaussian(key_of[5], (SEQS, SEQ_LEN, D), 1.0, 6.0, ((0, 4), (1, 8)))
    conv_x = gaussian(key_of[6], (CONV, D), CONV ** -0.5, 2.0, ((1, 8),), jnp.float32)
    conv_b = gaussian(key_of[7], (CONV, GROUPS * STATE), CONV ** -0.5, 2.0, ((1, 8),), jnp.float32)
    conv_c = gaussian(key_of[8], (CONV, GROUPS * STATE), CONV ** -0.5, 2.0, ((1, 8),), jnp.float32)
    decay_rate = draw_decay_rate(jax.random.fold_in(key_of[18], 71), 0)
    mix_gain = jnp.clip(1.0 + 0.18 * jax.random.normal(key_of[10], (D,), jnp.float32), 0.1, 1.9)
    out_weight = gaussian(key_of[11], (D, D), D ** -0.5, 0.125, ((0, 4),))
    ffn_gain = jnp.clip(1.0 + 0.18 * jax.random.normal(key_of[12], (D,), jnp.float32), 0.1, 1.9)
    routing_keys = jax.random.split(jax.random.fold_in(key_of[13], 1), SEQS * SEQ_LEN // TOK_DEV)
    routing_turns = jax.random.permutation(jax.random.fold_in(key_of[13], 3), SEQS * SEQ_LEN // TOK_DEV)
    routing = jax.vmap(lambda own, number: shared_out(jax.random.fold_in(key_of[13], 2), own, number, TOK_DEV, EXPERTS, TOPK, CAP, 2))(routing_keys, routing_turns).reshape((SEQS, SEQ_LEN, TOPK))
    route_weight = jnp.clip(0.1 + 0.5 * jax.random.uniform(key_of[14], (SEQS, SEQ_LEN, TOPK), jnp.float32) ** steps_of(key_of[14], (SEQS, SEQ_LEN, TOPK), ((0, 4), (1, 8)), -0.2, 0.2), 0.1, 0.6)
    gate_w = draw_gate_w(jax.random.fold_in(key_of[18], 71), 0)
    up_w = draw_up_w(jax.random.fold_in(key_of[18], 71), 0)
    down_w = gaussian(key_of[17], (EXPERTS, FF, D), FF ** -0.5, 0.1875, ((0, 32),))
    return {"residual_in": residual_in, "ssm_input": ssm_input, "state_b": state_b, "state_c": state_c, "step_raw": step_raw, "gate_input": gate_input, "conv_x": conv_x, "conv_b": conv_b, "conv_c": conv_c, "decay_rate": decay_rate, "mix_gain": mix_gain, "out_weight": out_weight, "ffn_gain": ffn_gain, "routing": routing, "route_weight": route_weight, "gate_w": gate_w, "up_w": up_w, "down_w": down_w}


highest = lax.Precision.HIGHEST
epsilon = 1e-05
clamp_limit = 7.0
sigmoid_slope = 1.702
group_rows = 256

def centred_conv(values, taps):
    half_width = taps.shape[0] // 2
    padded = jnp.pad(values, ((half_width, half_width), (0, 0)))
    total = jnp.zeros_like(values)
    for offset in range(taps.shape[0]):
        total = total + padded[offset:offset + values.shape[0]] * taps[offset]
    return total

def ssd_direction(signal, step_size, rates, write_map, read_map):
    length = signal.shape[0]
    head_count = signal.shape[1]
    head_width = signal.shape[2]
    group_count = write_map.shape[1]
    state_width = write_map.shape[2]
    per_group = head_count // group_count
    blocks = length // BLOCK
    scaled = (signal * step_size[..., None]).reshape(blocks, BLOCK, group_count, per_group, head_width)
    cumulative = jnp.cumsum((-step_size * rates).reshape(blocks, BLOCK, group_count, per_group), axis=1)
    write_block = write_map.reshape(blocks, BLOCK, group_count, state_width)
    read_block = read_map.reshape(blocks, BLOCK, group_count, state_width)
    spread = cumulative[:, :, None] - cumulative[:, None]
    lower_mask = (lax.iota(jnp.int32, BLOCK)[:, None] >= lax.iota(jnp.int32, BLOCK)[None, :])[None, :, :, None, None]
    weight_in = jnp.exp(jnp.where(lower_mask, spread, -jnp.inf))
    intersect = jnp.einsum('clgn,csgn->clsg', read_block, write_block, precision=highest)
    inside = jnp.einsum('clsgk,csgkp->clgkp', intersect[..., None] * weight_in, scaled, precision=highest)
    to_end = jnp.exp(cumulative[:, -1:] - cumulative)
    states = jnp.einsum('csgn,csgkp->cgkpn', write_block, scaled * to_end[..., None], precision=highest)
    carry_decay = jnp.exp(cumulative[:, -1])

    def advance(running, block_pair):
        block_state, factor = block_pair
        return (factor[..., None, None] * running + block_state, running)
    initial = jnp.zeros((group_count, per_group, head_width, state_width), jnp.float32)
    _, entering = lax.scan(advance, initial, (states, carry_decay))
    carried = jnp.einsum('clgn,cgkpn->clgkp', read_block, entering, precision=highest) * jnp.exp(cumulative)[..., None]
    return (inside + carried).reshape(length, head_count, head_width)

def both_ways(signal, steps_fwd, steps_bwd, rates, write_map, read_map):
    forward = ssd_direction(signal, steps_fwd, rates[0], write_map, read_map)
    backward = ssd_direction(jnp.flip(signal, 0), jnp.flip(steps_bwd, 0), rates[1], jnp.flip(write_map, 0), jnp.flip(read_map, 0))
    return forward + jnp.flip(backward, 0)

def scale_rows(values, gains):
    return values * lax.rsqrt(lax.optimization_barrier(jnp.mean(values * values, axis=-1, keepdims=True)) + epsilon) * gains

def group_scale(values, gains):
    shaped = values.reshape(values.shape[:-1] + (NORM_GROUPS, values.shape[-1] // NORM_GROUPS))
    shaped = shaped * lax.rsqrt(lax.optimization_barrier(jnp.mean(shaped * shaped, axis=-1, keepdims=True)) + epsilon)
    return shaped.reshape(values.shape) * gains

def expert_apply(rows, gate_mat, up_mat, down_mat):
    gate_value = jnp.minimum(jnp.dot(rows, gate_mat, preferred_element_type=jnp.float32), clamp_limit)
    up_value = jnp.clip(jnp.dot(rows, up_mat, preferred_element_type=jnp.float32), -clamp_limit, clamp_limit)
    active = ((up_value + 1.0) * gate_value * jax.nn.sigmoid(sigmoid_slope * gate_value)).astype(jnp.bfloat16)
    return jnp.dot(active, down_mat, preferred_element_type=jnp.float32).astype(jnp.bfloat16)

def reference(residual_in, ssm_input, state_b, state_c, step_raw, gate_input, conv_x, conv_b, conv_c, decay_rate, mix_gain, out_weight, ffn_gain, routing, route_weight, gate_w, up_w, down_w):

    def mix_sequence(operands):
        signal_in, write_in, read_in, step_in = operands
        length = signal_in.shape[0]
        signal = jax.nn.silu(centred_conv(signal_in.astype(jnp.float32), conv_x)).reshape(length, HEADS, HEAD_DIM)
        write_map = jax.nn.silu(centred_conv(write_in.astype(jnp.float32), conv_b)).reshape(length, GROUPS, STATE)
        read_map = jax.nn.silu(centred_conv(read_in.astype(jnp.float32), conv_c)).reshape(length, GROUPS, STATE)
        step_pair = jax.nn.softplus(step_in.astype(jnp.float32).reshape(length, HEADS, 2))
        result = both_ways(signal, step_pair[..., 0], step_pair[..., 1], decay_rate, write_map, read_map)
        return result.reshape(length, D).astype(jnp.bfloat16)
    mixed_heads = lax.map(mix_sequence, (ssm_input, state_b, state_c, step_raw))
    gated = mixed_heads.astype(jnp.float32) * jax.nn.silu(gate_input.astype(jnp.float32))
    mixed = group_scale(gated, mix_gain).astype(jnp.bfloat16).reshape(-1, D)
    stream = residual_in.reshape(-1, D).astype(jnp.float32) + jnp.dot(mixed, out_weight, preferred_element_type=jnp.float32)
    ffn_input = scale_rows(stream, ffn_gain).astype(jnp.bfloat16)
    flat_expert = routing.reshape(-1).astype(jnp.int32)
    assigned = flat_expert.shape[0]
    flat_token = lax.iota(jnp.int32, assigned) // TOPK
    flat_weight = route_weight.reshape(-1)
    order = jnp.argsort(flat_expert, stable=True).astype(jnp.int32)
    sorted_expert = flat_expert[order]
    counts = jnp.bincount(flat_expert, length=EXPERTS).astype(jnp.int32)
    padded = (counts + group_rows - 1) // group_rows * group_rows
    group_start = jnp.cumsum(counts).astype(jnp.int32) - counts
    padded_end = jnp.cumsum(padded).astype(jnp.int32)
    padded_start = padded_end - padded
    target = padded_start[sorted_expert] + (lax.iota(jnp.int32, assigned) - group_start[sorted_expert])
    block_count = (assigned + EXPERTS * (group_rows - 1)) // group_rows + 1
    total_rows = block_count * group_rows
    row_token = jnp.zeros((total_rows,), jnp.int32).at[target].set(flat_token[order])
    row_weight = jnp.zeros((total_rows,), jnp.float32).at[target].set(flat_weight[order])
    block_expert = jnp.minimum(jnp.searchsorted(padded_end, lax.iota(jnp.int32, block_count) * group_rows, side='right'), EXPERTS - 1).astype(jnp.int32)

    def run_block(routed, block_pair):
        block_index, expert_id = block_pair
        rows_token = lax.dynamic_slice_in_dim(row_token, block_index * group_rows, group_rows)
        rows_weight = lax.dynamic_slice_in_dim(row_weight, block_index * group_rows, group_rows)
        answer = expert_apply(ffn_input[rows_token], gate_w[expert_id], up_w[expert_id], down_w[expert_id])
        return (routed.at[rows_token].add(answer.astype(jnp.float32) * rows_weight[:, None]), None)
    routed_init = jnp.zeros(stream.shape, jnp.float32)
    routed, _ = lax.scan(run_block, routed_init, (lax.iota(jnp.int32, block_count), block_expert))
    return (stream + routed).astype(jnp.bfloat16).reshape(SEQS, SEQ_LEN, D)
```

```python
import jax
import jax.numpy as jnp
from jax import lax
from jax.experimental import pallas as pl
from jax.experimental.pallas import tpu as pltpu
from jax.sharding import PartitionSpec as P

HEAD_DIM = 64
STATE = 128
NORM_GROUPS = 4
STEP_ROWS = 16

highest = lax.Precision.HIGHEST
epsilon = 1e-05
clamp_limit = 7.0
sigmoid_slope = 1.702
f32 = jnp.float32
bf16 = jnp.bfloat16


def pack_body(x_ref, b_ref, c_ref, s_ref, o_ref):
    tokens = x_ref.shape[0]
    o_ref[0, :tokens] = x_ref[...]
    o_ref[0, tokens : 2 * tokens] = b_ref[...]
    o_ref[0, 2 * tokens : 3 * tokens] = c_ref[...]
    o_ref[0, 3 * tokens :] = jnp.zeros((STEP_ROWS, o_ref.shape[2]), bf16)
    o_ref[0, 3 * tokens :, :tokens] = s_ref[0]


def pack_inputs(x, b, c, steps, parts):
    tokens, width = x.shape
    part_width = width // parts
    column = pl.BlockSpec((tokens, part_width), lambda i: (0, i))
    rows = 3 * tokens + STEP_ROWS
    return pl.pallas_call(
        pack_body,
        grid=(parts,),
        in_specs=[column, column, column, pl.BlockSpec((1, STEP_ROWS, tokens), lambda i: (i, 0, 0))],
        out_specs=pl.BlockSpec((1, rows, part_width), lambda i: (i, 0, 0)),
        out_shape=jax.ShapeDtypeStruct((parts, rows, part_width), bf16),
        name="pack_inputs",
    )(x, b, c, steps)


def nt_dot(left, right):
    return lax.dot_general(left, right, (((1,), (1,)), ((), ())), preferred_element_type=f32)


def tn_dot(left, right):
    return lax.dot_general(left, right, (((0,), (0,)), ((), ())), preferred_element_type=f32)


def silu(x):
    return x * (1.0 / (1.0 + jnp.exp(-x)))


def mixer_body(
    in_ref, tx_ref, tb_ref, tc_ref, rate_ref, o_ref, pad_ref, sig_ref, wr_ref, rd_ref, col_ref,
    acc_ref, fwd_ref, bwd_ref,
):
    blocks, tokens, width = o_ref.shape
    groups = width // STATE
    heads = width // HEAD_DIM
    per_group = heads // groups
    taps = tx_ref.shape[0]
    half = taps // 2
    margin = 8
    length = blocks * tokens

    for i in range(3):
        pad_ref[i, :margin] = jnp.zeros((margin, width), f32)
        pad_ref[i, margin + length :] = jnp.zeros((margin, width), f32)

    def widen(c, _):
        for i in range(3):
            pad_ref[i, pl.ds(pl.multiple_of(c * tokens, tokens) + margin, tokens)] = in_ref[
                c, i * tokens : (i + 1) * tokens
            ].astype(f32)
        return 0

    lax.fori_loop(0, blocks, widen, 0)
    fwd_ref[...] = jnp.zeros(fwd_ref.shape, f32)
    bwd_ref[...] = jnp.zeros(bwd_ref.shape, f32)
    row_id = lax.broadcasted_iota(jnp.int32, (tokens, tokens), 0)
    col_id = lax.broadcasted_iota(jnp.int32, (tokens, tokens), 1)
    lower = row_id >= col_id
    upper = row_id <= col_id
    upto = jnp.where(upper, 1.0, 0.0).astype(f32)
    rates = rate_ref[...]
    lane = lax.broadcasted_iota(jnp.int32, (tokens, STATE), 1) // HEAD_DIM

    def conv(i, c, tap_ref):
        window = pad_ref[i, pl.ds(pl.multiple_of(c * tokens, tokens), tokens + 2 * margin)]
        total = window[margin - half : margin - half + tokens] * tap_ref[0:1]
        for j in range(1, taps):
            first = margin - half + j
            total = total + window[first : first + tokens] * tap_ref[j : j + 1]
        return silu(total)

    def spread_heads(cols, g):
        wide = jnp.broadcast_to(cols[g * per_group], (tokens, STATE))
        for k in range(1, per_group):
            wide = jnp.where(
                lane == k, jnp.broadcast_to(cols[g * per_group + k], (tokens, STATE)), wide
            )
        return wide

    def forward(c, _):
        at = pl.ds(pl.multiple_of(c * tokens, tokens), tokens)
        signal = conv(0, c, tx_ref)
        write = conv(1, c, tb_ref).astype(bf16)
        read = conv(2, c, tc_ref).astype(bf16)
        sig_ref[at] = signal
        wr_ref[at] = write
        rd_ref[at] = read
        raw = in_ref[c, 3 * tokens : 3 * tokens + STEP_ROWS, :tokens].astype(f32)
        step = jnp.maximum(raw, 0.0) + jnp.log1p(jnp.exp(-jnp.abs(raw)))
        drop = step * rates
        incl = jnp.dot(drop, upto, precision=highest, preferred_element_type=f32)
        excl = incl - drop
        stacked = jnp.concatenate(
            [incl, excl, step, jnp.zeros((tokens - 3 * STEP_ROWS, tokens), f32)], axis=0
        )
        cols = stacked.T
        col_ref[at] = cols

        def col(kind, row):
            return cols[:, kind * STEP_ROWS + row : kind * STEP_ROWS + row + 1]

        signal_b = signal.astype(bf16)
        reach = [col(0, 2 * h) for h in range(heads)]
        last = [incl[2 * h : 2 * h + 1, tokens - 1 : tokens] for h in range(heads)]
        scale = [col(2, 2 * h) * jnp.exp(reach[h] - last[h]) for h in range(heads)]
        fade = [jnp.exp(-reach[h]) for h in range(heads)]
        keep = [jnp.broadcast_to(jnp.exp(-last[h]), (tokens, 1)) for h in range(heads)]
        for g in range(groups):
            lanes = slice(g * STATE, (g + 1) * STATE)
            read_g = read[:, lanes]
            write_g = write[:, lanes]
            match = nt_dot(read_g, write_g)
            pieces = []
            for h in range(g * per_group, (g + 1) * per_group):
                f, b = 2 * h, 2 * h + 1
                gap = jnp.where(
                    lower, incl[f : f + 1] - reach[h], col(1, b) - excl[b : b + 1]
                )
                weight = jnp.exp(gap) * (
                    jnp.where(lower, step[f : f + 1], 0.0) + jnp.where(upper, step[b : b + 1], 0.0)
                )
                pieces.append(
                    jnp.dot(
                        (match * weight).astype(bf16),
                        signal_b[:, h * HEAD_DIM : (h + 1) * HEAD_DIM],
                        preferred_element_type=f32,
                    )
                )
            state = fwd_ref[g]
            carried = jnp.dot(read_g, state.astype(bf16), preferred_element_type=f32)
            acc_ref[at, lanes] = jnp.concatenate(pieces, axis=1) + carried * spread_heads(fade, g)
            fresh = tn_dot(write_g, (signal[:, lanes] * spread_heads(scale, g)).astype(bf16))
            fwd_ref[g] = state * spread_heads(keep, g) + fresh
        return 0

    lax.fori_loop(0, blocks, forward, 0)

    def backward(i, _):
        c = blocks - 1 - i
        at = pl.ds(pl.multiple_of(c * tokens, tokens), tokens)
        cols = col_ref[at]
        signal = sig_ref[at]
        write = wr_ref[at]
        read = rd_ref[at]

        def col(kind, row):
            return cols[:, kind * STEP_ROWS + row : kind * STEP_ROWS + row + 1]

        ahead = [col(1, 2 * h + 1) for h in range(heads)]
        whole = [col(0, 2 * h + 1)[tokens - 1 : tokens] for h in range(heads)]
        scale = [col(2, 2 * h + 1) * jnp.exp(-ahead[h]) for h in range(heads)]
        fade = [jnp.exp(ahead[h] - whole[h]) for h in range(heads)]
        keep = [jnp.broadcast_to(jnp.exp(-whole[h]), (tokens, 1)) for h in range(heads)]
        for g in range(groups):
            lanes = slice(g * STATE, (g + 1) * STATE)
            state = bwd_ref[g]
            carried = jnp.dot(read[:, lanes], state.astype(bf16), preferred_element_type=f32)
            o_ref[c, :, lanes] = (acc_ref[at, lanes] + carried * spread_heads(fade, g)).astype(bf16)
            fresh = tn_dot(write[:, lanes], (signal[:, lanes] * spread_heads(scale, g)).astype(bf16))
            bwd_ref[g] = state * spread_heads(keep, g) + fresh
        return 0

    lax.fori_loop(0, blocks, backward, 0)


def mixer(arrived, conv_x, conv_b, conv_c, decay_rate):
    blocks, rows, width = arrived.shape
    tokens = (rows - STEP_ROWS) // 3
    length = blocks * tokens
    groups = width // STATE
    rates = decay_rate.T.reshape(-1, 1)
    rates = jnp.pad(rates, ((0, STEP_ROWS - rates.shape[0]), (0, 0)))
    return pl.pallas_call(
        mixer_body,
        out_shape=jax.ShapeDtypeStruct((blocks, tokens, width), bf16),
        scratch_shapes=[
            pltpu.VMEM((3, length + 16, width), f32),
            pltpu.VMEM((length, width), f32),
            pltpu.VMEM((length, width), bf16),
            pltpu.VMEM((length, width), bf16),
            pltpu.VMEM((length, tokens), f32),
            pltpu.VMEM((length, width), f32),
            pltpu.VMEM((groups, STATE, STATE), f32),
            pltpu.VMEM((groups, STATE, STATE), f32),
        ],
        compiler_params=pltpu.CompilerParams(vmem_limit_bytes=32 * 1024 * 1024),
        name="mixer",
    )(arrived, conv_x, conv_b, conv_c, rates)


def project_body(
    mix_ref, gate_ref, gain_ref, w_ref, res_ref, fgain_ref, sel_ref, stream_ref, out_ref, mixed_ref
):
    n = pl.program_id(0)
    parts, tokens, part_width = mix_ref.shape
    model = gate_ref.shape[1]
    span = model // NORM_GROUPS
    each = span // part_width
    block = w_ref.shape[1]

    @pl.when(n == 0)
    def _():
        for q in range(NORM_GROUPS):
            piece = jnp.concatenate([mix_ref[q * each + i] for i in range(each)], axis=1)
            cols = slice(q * span, (q + 1) * span)
            value = piece.astype(f32) * silu(gate_ref[:, cols].astype(f32))
            norm = lax.rsqrt(jnp.mean(value * value, axis=-1, keepdims=True) + epsilon)
            mixed_ref[:, cols] = (value * norm * gain_ref[:, cols]).astype(bf16)

    stream_ref[:, pl.ds(pl.multiple_of(n * block, block), block)] = res_ref[...].astype(
        f32
    ) + jnp.dot(mixed_ref[...], w_ref[...], preferred_element_type=f32)

    @pl.when(n == pl.num_programs(0) - 1)
    def _():
        stream = stream_ref[...]
        norm = lax.rsqrt(jnp.mean(stream * stream, axis=-1, keepdims=True) + epsilon)
        rows = (stream * norm * fgain_ref[...]).astype(bf16)
        out_ref[...] = jnp.dot(sel_ref[...], rows, preferred_element_type=f32).astype(bf16)


def project(mix, gate, gain, weight, residual, fgain, select):
    tokens, model = gate.shape
    block = model // 4
    slots = select.shape[0]

    def whole(shape):
        return pl.BlockSpec(shape, lambda n: (0,) * len(shape))

    return pl.pallas_call(
        project_body,
        grid=(model // block,),
        in_specs=[
            whole(mix.shape),
            whole(gate.shape),
            whole((1, model)),
            pl.BlockSpec((model, block), lambda n: (0, n)),
            pl.BlockSpec((tokens, block), lambda n: (0, n)),
            whole((1, model)),
            whole(select.shape),
        ],
        out_specs=[whole((tokens, model)), whole((slots, model))],
        out_shape=[
            jax.ShapeDtypeStruct((tokens, model), f32),
            jax.ShapeDtypeStruct((slots, model), bf16),
        ],
        scratch_shapes=[pltpu.VMEM((tokens, model), bf16)],
        compiler_params=pltpu.CompilerParams(vmem_limit_bytes=48 * 1024 * 1024),
        name="project",
    )(mix, gate, gain.reshape(1, -1), weight, residual, fgain.reshape(1, -1), select)


def expert_apply(rows, gate_mat, up_mat, down_mat):
    gate_value = jnp.minimum(
        jnp.dot(rows, gate_mat, preferred_element_type=jnp.float32), clamp_limit
    )
    up_value = jnp.clip(
        jnp.dot(rows, up_mat, preferred_element_type=jnp.float32), -clamp_limit, clamp_limit
    )
    active = ((up_value + 1.0) * gate_value * jax.nn.sigmoid(sigmoid_slope * gate_value)).astype(
        jnp.bfloat16
    )
    return jnp.dot(active, down_mat, preferred_element_type=jnp.float32).astype(jnp.bfloat16)


def per_device(
    residual_in,
    ssm_input,
    state_b,
    state_c,
    step_raw,
    gate_input,
    conv_x,
    conv_b,
    conv_c,
    decay_rate,
    mix_gain,
    out_weight,
    ffn_gain,
    routing,
    route_weight,
    gate_w,
    up_w,
    down_w,
):
    sp_count = lax.axis_size("sp")
    dp_count = lax.axis_size("dp")
    experts_all = sp_count * dp_count
    token_count = residual_in.shape[1]
    model_width = residual_in.shape[2]
    top_count = routing.shape[2]
    capacity = 2 * token_count * top_count // experts_all

    steps = step_raw[0].T.reshape(sp_count, -1, token_count)
    steps = jnp.pad(steps, ((0, 0), (0, STEP_ROWS - steps.shape[1]), (0, 0)))
    packed = pack_inputs(ssm_input[0], state_b[0], state_c[0], steps, sp_count)
    arrived_mix = lax.all_to_all(packed, "sp", split_axis=0, concat_axis=0, tiled=True)
    mixed_heads = mixer(arrived_mix, conv_x, conv_b, conv_c, decay_rate)
    mixed_tokens = lax.all_to_all(mixed_heads, "sp", split_axis=0, concat_axis=0, tiled=True)

    routes = routing[0]
    hits = routes.T[:, None, :] == lax.iota(jnp.int32, experts_all)[None, :, None]
    mask = jnp.any(hits, axis=0)
    share = jnp.sum(jnp.where(hits, route_weight[0].T[:, None, :], 0.0), axis=0)
    earlier = (
        lax.iota(jnp.int32, token_count)[:, None] < lax.iota(jnp.int32, token_count)[None, :]
    ).astype(bf16)
    rank = jnp.dot(mask.astype(bf16), earlier, preferred_element_type=f32).astype(jnp.int32)
    rank = jnp.where(mask, rank, capacity)
    chosen = rank[:, None, :] == lax.iota(jnp.int32, capacity)[None, :, None]
    select = chosen.astype(bf16).reshape(experts_all * capacity, token_count)
    share_top = share.astype(bf16)
    share_rest = (share - share_top.astype(f32)).astype(bf16)
    shares = jnp.stack([share_top, share_rest])
    merge = jnp.where(chosen[None], shares[:, :, None, :], jnp.zeros((), bf16)).reshape(
        2, experts_all * capacity, token_count
    )

    stream, outgoing = project(
        mixed_tokens,
        gate_input[0],
        mix_gain,
        lax.all_gather(out_weight, "dp", axis=0, tiled=True),
        residual_in[0],
        ffn_gain,
        select,
    )
    arrived = lax.all_to_all(
        outgoing.reshape(experts_all, capacity, model_width),
        ("sp", "dp"),
        split_axis=0,
        concat_axis=0,
        tiled=True,
    )
    served = expert_apply(arrived.reshape(-1, model_width), gate_w[0], up_w[0], down_w[0]).reshape(
        arrived.shape
    )
    returned = lax.all_to_all(served, ("sp", "dp"), split_axis=0, concat_axis=0, tiled=True)
    routed = jnp.einsum(
        "ast,sd->atd",
        merge,
        returned.reshape(experts_all * capacity, model_width),
        preferred_element_type=f32,
    )
    return (stream + routed[0] + routed[1]).astype(bf16)[None]


def solution(mesh):
    return jax.shard_map(
        per_device,
        mesh=mesh,
        in_specs=(
            P("dp", "sp", None),
            P("dp", "sp", None),
            P("dp", "sp", None),
            P("dp", "sp", None),
            P("dp", "sp", None),
            P("dp", "sp", None),
            P(None, "sp"),
            P(None, "sp"),
            P(None, "sp"),
            P(None, "sp"),
            P(),
            P("dp", None),
            P(),
            P("dp", "sp", None),
            P("dp", "sp", None),
            P(("sp", "dp"), None, None),
            P(("sp", "dp"), None, None),
            P(("sp", "dp"), None, None),
        ),
        out_specs=P("dp", "sp", None),
        check_vma=False,
    )
```

```python
import jax
import jax.numpy as jnp
from jax import lax
from jax.experimental import pallas as pl
from jax.experimental.pallas import tpu as pltpu
from jax.sharding import PartitionSpec as P

HEAD_DIM = 64
STATE = 128
NORM_GROUPS = 4
STEP_ROWS = 16

highest = lax.Precision.HIGHEST
epsilon = 1e-05
clamp_limit = 7.0
sigmoid_slope = 1.702
f32 = jnp.float32
bf16 = jnp.bfloat16


def pack_body(x_ref, b_ref, c_ref, s_ref, o_ref):
    tokens = x_ref.shape[0]
    o_ref[0, :tokens] = x_ref[...]
    o_ref[0, tokens : 2 * tokens] = b_ref[...]
    o_ref[0, 2 * tokens : 3 * tokens] = c_ref[...]
    o_ref[0, 3 * tokens :] = jnp.zeros((STEP_ROWS, o_ref.shape[2]), bf16)
    o_ref[0, 3 * tokens :, :tokens] = s_ref[0]


def pack_inputs(x, b, c, steps, parts):
    tokens, width = x.shape
    part_width = width // parts
    column = pl.BlockSpec((tokens, part_width), lambda i: (0, i))
    rows = 3 * tokens + STEP_ROWS
    return pl.pallas_call(
        pack_body,
        grid=(parts,),
        in_specs=[column, column, column, pl.BlockSpec((1, STEP_ROWS, tokens), lambda i: (i, 0, 0))],
        out_specs=pl.BlockSpec((1, rows, part_width), lambda i: (i, 0, 0)),
        out_shape=jax.ShapeDtypeStruct((parts, rows, part_width), bf16),
        name="pack_inputs",
    )(x, b, c, steps)


def nt_dot(left, right):
    return lax.dot_general(left, right, (((1,), (1,)), ((), ())), preferred_element_type=f32)


def tn_dot(left, right):
    return lax.dot_general(left, right, (((0,), (0,)), ((), ())), preferred_element_type=f32)


def silu(x):
    return x * (1.0 / (1.0 + jnp.exp(-x)))


def mixer_body(
    in_ref, tx_ref, tb_ref, tc_ref, rate_ref, o_ref, pad_ref, sig_ref, wr_ref, rd_ref, col_ref,
    acc_ref, fwd_ref, bwd_ref,
):
    blocks, tokens, width = o_ref.shape
    groups = width // STATE
    heads = width // HEAD_DIM
    per_group = heads // groups
    taps = tx_ref.shape[0]
    half = taps // 2
    margin = 8
    length = blocks * tokens

    for i in range(3):
        pad_ref[i, :margin] = jnp.zeros((margin, width), f32)
        pad_ref[i, margin + length :] = jnp.zeros((margin, width), f32)

    def widen(c, _):
        for i in range(3):
            pad_ref[i, pl.ds(pl.multiple_of(c * tokens, tokens) + margin, tokens)] = in_ref[
                c, i * tokens : (i + 1) * tokens
            ].astype(f32)
        return 0

    lax.fori_loop(0, blocks, widen, 0)
    fwd_ref[...] = jnp.zeros(fwd_ref.shape, f32)
    bwd_ref[...] = jnp.zeros(bwd_ref.shape, f32)
    row_id = lax.broadcasted_iota(jnp.int32, (tokens, tokens), 0)
    col_id = lax.broadcasted_iota(jnp.int32, (tokens, tokens), 1)
    lower = row_id >= col_id
    upper = row_id <= col_id
    upto = jnp.where(upper, 1.0, 0.0).astype(f32)
    rates = rate_ref[...]
    lane = lax.broadcasted_iota(jnp.int32, (tokens, STATE), 1) // HEAD_DIM

    def conv(i, c, tap_ref):
        window = pad_ref[i, pl.ds(pl.multiple_of(c * tokens, tokens), tokens + 2 * margin)]
        total = window[margin - half : margin - half + tokens] * tap_ref[0:1]
        for j in range(1, taps):
            first = margin - half + j
            total = total + window[first : first + tokens] * tap_ref[j : j + 1]
        return silu(total)

    def spread_heads(cols, g):
        wide = jnp.broadcast_to(cols[g * per_group], (tokens, STATE))
        for k in range(1, per_group):
            wide = jnp.where(
                lane == k, jnp.broadcast_to(cols[g * per_group + k], (tokens, STATE)), wide
            )
        return wide

    def forward(c, _):
        at = pl.ds(pl.multiple_of(c * tokens, tokens), tokens)
        signal = conv(0, c, tx_ref)
        write = conv(1, c, tb_ref).astype(bf16)
        read = conv(2, c, tc_ref).astype(bf16)
        sig_ref[at] = signal
        wr_ref[at] = write
        rd_ref[at] = read
        raw = in_ref[c, 3 * tokens : 3 * tokens + STEP_ROWS, :tokens].astype(f32)
        step = jnp.maximum(raw, 0.0) + jnp.log1p(jnp.exp(-jnp.abs(raw)))
        drop = step * rates
        incl = jnp.dot(drop, upto, precision=highest, preferred_element_type=f32)
        excl = incl - drop
        stacked = jnp.concatenate(
            [incl, excl, step, jnp.zeros((tokens - 3 * STEP_ROWS, tokens), f32)], axis=0
        )
        cols = stacked.T
        col_ref[at] = cols

        def col(kind, row):
            return cols[:, kind * STEP_ROWS + row : kind * STEP_ROWS + row + 1]

        signal_b = signal.astype(bf16)
        reach = [col(0, 2 * h) for h in range(heads)]
        last = [incl[2 * h : 2 * h + 1, tokens - 1 : tokens] for h in range(heads)]
        scale = [col(2, 2 * h) * jnp.exp(reach[h] - last[h]) for h in range(heads)]
        fade = [jnp.exp(-reach[h]) for h in range(heads)]
        keep = [jnp.broadcast_to(jnp.exp(-last[h]), (tokens, 1)) for h in range(heads)]
        for g in range(groups):
            lanes = slice(g * STATE, (g + 1) * STATE)
            read_g = read[:, lanes]
            write_g = write[:, lanes]
            match = nt_dot(read_g, write_g)
            pieces = []
            for h in range(g * per_group, (g + 1) * per_group):
                f, b = 2 * h, 2 * h + 1
                gap = jnp.where(
                    lower, incl[f : f + 1] - reach[h], col(1, b) - excl[b : b + 1]
                )
                weight = jnp.exp(gap) * (
                    jnp.where(lower, step[f : f + 1], 0.0) + jnp.where(upper, step[b : b + 1], 0.0)
                )
                pieces.append(
                    jnp.dot(
                        (match * weight).astype(bf16),
                        signal_b[:, h * HEAD_DIM : (h + 1) * HEAD_DIM],
                        preferred_element_type=f32,
                    )
                )
            state = fwd_ref[g]
            carried = jnp.dot(read_g, state.astype(bf16), preferred_element_type=f32)
            acc_ref[at, lanes] = jnp.concatenate(pieces, axis=1) + carried * spread_heads(fade, g)
            fresh = tn_dot(write_g, (signal[:, lanes] * spread_heads(scale, g)).astype(bf16))
            fwd_ref[g] = state * spread_heads(keep, g) + fresh
        return 0

    lax.fori_loop(0, blocks, forward, 0)

    def backward(i, _):
        c = blocks - 1 - i
        at = pl.ds(pl.multiple_of(c * tokens, tokens), tokens)
        cols = col_ref[at]
        signal = sig_ref[at]
        write = wr_ref[at]
        read = rd_ref[at]

        def col(kind, row):
            return cols[:, kind * STEP_ROWS + row : kind * STEP_ROWS + row + 1]

        ahead = [col(1, 2 * h + 1) for h in range(heads)]
        whole = [col(0, 2 * h + 1)[tokens - 1 : tokens] for h in range(heads)]
        scale = [col(2, 2 * h + 1) * jnp.exp(-ahead[h]) for h in range(heads)]
        fade = [jnp.exp(ahead[h] - whole[h]) for h in range(heads)]
        keep = [jnp.broadcast_to(jnp.exp(-whole[h]), (tokens, 1)) for h in range(heads)]
        for g in range(groups):
            lanes = slice(g * STATE, (g + 1) * STATE)
            state = bwd_ref[g]
            carried = jnp.dot(read[:, lanes], state.astype(bf16), preferred_element_type=f32)
            o_ref[c, :, lanes] = (acc_ref[at, lanes] + carried * spread_heads(fade, g)).astype(bf16)
            fresh = tn_dot(write[:, lanes], (signal[:, lanes] * spread_heads(scale, g)).astype(bf16))
            bwd_ref[g] = state * spread_heads(keep, g) + fresh
        return 0

    lax.fori_loop(0, blocks, backward, 0)


def mixer(arrived, conv_x, conv_b, conv_c, decay_rate):
    blocks, rows, width = arrived.shape
    tokens = (rows - STEP_ROWS) // 3
    length = blocks * tokens
    groups = width // STATE
    rates = decay_rate.T.reshape(-1, 1)
    rates = jnp.pad(rates, ((0, STEP_ROWS - rates.shape[0]), (0, 0)))
    return pl.pallas_call(
        mixer_body,
        out_shape=jax.ShapeDtypeStruct((blocks, tokens, width), bf16),
        scratch_shapes=[
            pltpu.VMEM((3, length + 16, width), f32),
            pltpu.VMEM((length, width), f32),
            pltpu.VMEM((length, width), bf16),
            pltpu.VMEM((length, width), bf16),
            pltpu.VMEM((length, tokens), f32),
            pltpu.VMEM((length, width), f32),
            pltpu.VMEM((groups, STATE, STATE), f32),
            pltpu.VMEM((groups, STATE, STATE), f32),
        ],
        compiler_params=pltpu.CompilerParams(vmem_limit_bytes=32 * 1024 * 1024),
        name="mixer",
    )(arrived, conv_x, conv_b, conv_c, rates)


def project_body(place_ref, mix_ref, gate_ref, gain_ref, res_ref, fgain_ref, *rest):
    *w_refs, stream_ref, rows_ref, mixed_ref = rest
    n = pl.program_id(0)
    parts, tokens, part_width = mix_ref.shape
    model = gate_ref.shape[1]
    span = model // NORM_GROUPS
    each = span // part_width
    seg = mixed_ref.shape[2]
    unit = min(seg, span)
    block = w_refs[0].shape[1]

    @pl.when(n == 0)
    def _():
        for q in range(NORM_GROUPS):
            piece = jnp.concatenate([mix_ref[q * each + i] for i in range(each)], axis=1)
            cols = slice(q * span, (q + 1) * span)
            value = piece.astype(f32) * silu(gate_ref[:, cols].astype(f32))
            norm = lax.rsqrt(jnp.mean(value * value, axis=-1, keepdims=True) + epsilon)
            value = (value * norm * gain_ref[:, cols]).astype(bf16)
            for u in range(0, span, unit):
                at = q * span + u
                mixed_ref[at // seg, :, at % seg : at % seg + unit] = value[:, u : u + unit]

    total = res_ref[...].astype(f32)
    for m in range(len(w_refs)):
        total = total + jnp.dot(
            mixed_ref[place_ref[0] ^ m], w_refs[m][...], preferred_element_type=f32
        )
    stream_ref[:, pl.ds(pl.multiple_of(n * block, block), block)] = total

    @pl.when(n == pl.num_programs(0) - 1)
    def _():
        stream = stream_ref[...]
        norm = lax.rsqrt(jnp.mean(stream * stream, axis=-1, keepdims=True) + epsilon)
        rows = (stream * norm * fgain_ref[...]).astype(bf16)
        rows_ref[...] = rows


def project(place, mix, gate, gain, weights, residual, fgain):
    tokens, model = gate.shape
    block = model // 4
    seg = weights[0].shape[0]

    def whole(shape):
        return pl.BlockSpec(shape, lambda n: (0,) * len(shape))

    return pl.pallas_call(
        project_body,
        grid=(model // block,),
        in_specs=[
            pl.BlockSpec(memory_space=pltpu.SMEM),
            whole(mix.shape),
            whole(gate.shape),
            whole((1, model)),
            pl.BlockSpec((tokens, block), lambda n: (0, n)),
            whole((1, model)),
        ]
        + [pl.BlockSpec((seg, block), lambda n: (0, n))] * len(weights),
        out_specs=[whole((tokens, model)), whole((tokens, model))],
        out_shape=[
            jax.ShapeDtypeStruct((tokens, model), f32),
            jax.ShapeDtypeStruct((tokens, model), bf16),
        ],
        scratch_shapes=[pltpu.VMEM((model // seg, tokens, seg), bf16)],
        compiler_params=pltpu.CompilerParams(vmem_limit_bytes=48 * 1024 * 1024),
        name="project",
    )(place, mix, gate, gain.reshape(1, -1), residual, fgain.reshape(1, -1), *weights)


def slot_maps(routes, weights, first, experts, capacity):
    tokens = routes.shape[0]
    hits = routes.T[:, None, :] == (first + lax.iota(jnp.int32, experts))[None, :, None]
    mask = jnp.any(hits, axis=0)
    share = jnp.sum(jnp.where(hits, weights.T[:, None, :], 0.0), axis=0)
    earlier = (lax.iota(jnp.int32, tokens)[:, None] < lax.iota(jnp.int32, tokens)[None, :]).astype(
        bf16
    )
    rank = jnp.dot(mask.astype(bf16), earlier, preferred_element_type=f32).astype(jnp.int32)
    rank = jnp.where(mask, rank, capacity)
    chosen = rank[:, None, :] == lax.iota(jnp.int32, capacity)[None, :, None]
    select = chosen.astype(bf16).reshape(experts * capacity, tokens)
    share_top = share.astype(bf16)
    share_rest = (share - share_top.astype(f32)).astype(bf16)
    shares = jnp.stack([share_top, share_rest])
    merge = jnp.where(chosen[None], shares[:, :, None, :], jnp.zeros((), bf16)).reshape(
        2, experts * capacity, tokens
    )
    return select, merge


def weighted_sum(merge, answers):
    both = jnp.einsum("ast,sd->atd", merge, answers, preferred_element_type=f32)
    return both[0] + both[1]


def expert_apply(rows, gate_mat, up_mat, down_mat):
    gate_value = jnp.minimum(
        jnp.dot(rows, gate_mat, preferred_element_type=jnp.float32), clamp_limit
    )
    up_value = jnp.clip(
        jnp.dot(rows, up_mat, preferred_element_type=jnp.float32), -clamp_limit, clamp_limit
    )
    active = ((up_value + 1.0) * gate_value * jax.nn.sigmoid(sigmoid_slope * gate_value)).astype(
        jnp.bfloat16
    )
    return jnp.dot(active, down_mat, preferred_element_type=jnp.float32).astype(jnp.bfloat16)


def per_device(
    residual_in,
    ssm_input,
    state_b,
    state_c,
    step_raw,
    gate_input,
    conv_x,
    conv_b,
    conv_c,
    decay_rate,
    mix_gain,
    out_weight,
    ffn_gain,
    routing,
    route_weight,
    gate_w,
    up_w,
    down_w,
):
    sp_axes = ("half", "rest")
    group_axes = ("rest", "dp")
    sp_count = lax.axis_size(sp_axes)
    dp_count = lax.axis_size("dp")
    group = lax.axis_size(group_axes)
    experts_all = sp_count * dp_count
    token_count = residual_in.shape[1]
    model_width = residual_in.shape[2]
    top_count = routing.shape[2]
    capacity = 2 * token_count * top_count // experts_all
    swap = [(0, 1), (1, 0)]

    pieces = {0: out_weight}
    bit = dp_count // 2
    while bit:
        steps_of = [(i, i ^ bit) for i in range(dp_count)]
        fresh = {m ^ bit: lax.ppermute(piece, "dp", steps_of) for m, piece in pieces.items()}
        pieces.update(fresh)
        bit //= 2

    other_routes = lax.ppermute(routing[0], "half", swap)
    other_weight = lax.ppermute(route_weight[0], "half", swap)

    steps = step_raw[0].T.reshape(sp_count, -1, token_count)
    steps = jnp.pad(steps, ((0, 0), (0, STEP_ROWS - steps.shape[1]), (0, 0)))
    packed = pack_inputs(ssm_input[0], state_b[0], state_c[0], steps, sp_count)
    arrived_mix = lax.all_to_all(packed, sp_axes, split_axis=0, concat_axis=0, tiled=True)
    arrived_mix, other_routes, other_weight = lax.optimization_barrier(
        (arrived_mix, other_routes, other_weight)
    )
    mixed_heads = mixer(arrived_mix, conv_x, conv_b, conv_c, decay_rate)
    mixed_tokens = lax.all_to_all(mixed_heads, sp_axes, split_axis=0, concat_axis=0, tiled=True)

    first = lax.axis_index("half") * group
    select, merge = slot_maps(routing[0], route_weight[0], first, group, capacity)
    other_select, other_merge = slot_maps(other_routes, other_weight, first, group, capacity)

    stream, rows = project(
        lax.axis_index("dp").reshape(1),
        mixed_tokens,
        gate_input[0],
        mix_gain,
        [pieces[m] for m in range(dp_count)],
        residual_in[0],
        ffn_gain,
    )

    def exchange(slots):
        return lax.all_to_all(
            slots.reshape(group, capacity, model_width),
            group_axes,
            split_axis=0,
            concat_axis=0,
            tiled=True,
        ).reshape(group * capacity, model_width)

    other_rows = lax.ppermute(rows, "half", swap)
    arrived = exchange(jnp.dot(select, rows, preferred_element_type=f32).astype(bf16))
    other_rows, arrived = lax.optimization_barrier((other_rows, arrived))
    other_arrived = exchange(
        jnp.dot(other_select, other_rows, preferred_element_type=f32).astype(bf16)
    )
    served = expert_apply(arrived, gate_w[0], up_w[0], down_w[0])
    other_served = expert_apply(other_arrived, gate_w[0], up_w[0], down_w[0])
    other_answers = exchange(other_served)
    other_sum = weighted_sum(other_merge, other_answers).astype(bf16)
    served, other_sum = lax.optimization_barrier((served, other_sum))
    from_other = lax.ppermute(other_sum, "half", swap)
    answers = exchange(served)
    return (stream + weighted_sum(merge, answers) + from_other.astype(f32)).astype(bf16)[None]


def solution(mesh):
    devices = mesh.devices
    halves = jax.sharding.Mesh(
        devices.reshape(2, devices.shape[0] // 2, devices.shape[1]), ("half", "rest", "dp")
    )
    return jax.shard_map(
        per_device,
        mesh=halves,
        in_specs=(
            P("dp", ("half", "rest"), None),
            P("dp", ("half", "rest"), None),
            P("dp", ("half", "rest"), None),
            P("dp", ("half", "rest"), None),
            P("dp", ("half", "rest"), None),
            P("dp", ("half", "rest"), None),
            P(None, ("half", "rest")),
            P(None, ("half", "rest")),
            P(None, ("half", "rest")),
            P(None, ("half", "rest")),
            P(),
            P("dp", None),
            P(),
            P("dp", ("half", "rest"), None),
            P("dp", ("half", "rest"), None),
            P(("half", "rest", "dp"), None, None),
            P(("half", "rest", "dp"), None, None),
            P(("half", "rest", "dp"), None, None),
        ),
        out_specs=P("dp", ("half", "rest"), None),
        check_vma=False,
    )
```

```python
import jax
import jax.numpy as jnp
from jax import lax
from jax.experimental import pallas as pl
from jax.experimental.pallas import tpu as pltpu
from jax.sharding import PartitionSpec as P

HEAD_DIM = 64
STATE = 128
NORM_GROUPS = 4
STEP_ROWS = 16

highest = lax.Precision.HIGHEST
epsilon = 1e-05
clamp_limit = 7.0
sigmoid_slope = 1.702
f32 = jnp.float32
bf16 = jnp.bfloat16


def pack_body(x_ref, b_ref, c_ref, s_ref, o_ref):
    tokens = x_ref.shape[0]
    o_ref[0, :tokens] = x_ref[...]
    o_ref[0, tokens : 2 * tokens] = b_ref[...]
    o_ref[0, 2 * tokens : 3 * tokens] = c_ref[...]
    o_ref[0, 3 * tokens :] = jnp.zeros((STEP_ROWS, o_ref.shape[2]), bf16)
    o_ref[0, 3 * tokens :, :tokens] = s_ref[0]


def pack_inputs(x, b, c, steps, parts):
    tokens, width = x.shape
    part_width = width // parts
    column = pl.BlockSpec((tokens, part_width), lambda i: (0, i))
    rows = 3 * tokens + STEP_ROWS
    return pl.pallas_call(
        pack_body,
        grid=(parts,),
        in_specs=[column, column, column, pl.BlockSpec((1, STEP_ROWS, tokens), lambda i: (i, 0, 0))],
        out_specs=pl.BlockSpec((1, rows, part_width), lambda i: (i, 0, 0)),
        out_shape=jax.ShapeDtypeStruct((parts, rows, part_width), bf16),
        name="pack_inputs",
    )(x, b, c, steps)


def nt_dot(left, right):
    return lax.dot_general(left, right, (((1,), (1,)), ((), ())), preferred_element_type=f32)


def tn_dot(left, right):
    return lax.dot_general(left, right, (((0,), (0,)), ((), ())), preferred_element_type=f32)


def silu(x):
    return x * (1.0 / (1.0 + jnp.exp(-x)))


def mixer_body(
    in_ref, tx_ref, tb_ref, tc_ref, rate_ref, o_ref, pad_ref, sig_ref, wr_ref, rd_ref, col_ref,
    acc_ref, fwd_ref, bwd_ref,
):
    blocks, tokens, width = o_ref.shape
    groups = width // STATE
    heads = width // HEAD_DIM
    per_group = heads // groups
    taps = tx_ref.shape[0]
    half = taps // 2
    margin = 8
    length = blocks * tokens

    for i in range(3):
        pad_ref[i, :margin] = jnp.zeros((margin, width), f32)
        pad_ref[i, margin + length :] = jnp.zeros((margin, width), f32)

    def widen(c, _):
        for i in range(3):
            pad_ref[i, pl.ds(pl.multiple_of(c * tokens, tokens) + margin, tokens)] = in_ref[
                c, i * tokens : (i + 1) * tokens
            ].astype(f32)
        return 0

    lax.fori_loop(0, blocks, widen, 0)
    fwd_ref[...] = jnp.zeros(fwd_ref.shape, f32)
    bwd_ref[...] = jnp.zeros(bwd_ref.shape, f32)
    row_id = lax.broadcasted_iota(jnp.int32, (tokens, tokens), 0)
    col_id = lax.broadcasted_iota(jnp.int32, (tokens, tokens), 1)
    lower = row_id >= col_id
    upper = row_id <= col_id
    upto = jnp.where(upper, 1.0, 0.0).astype(f32)
    rates = rate_ref[...]
    lane = lax.broadcasted_iota(jnp.int32, (tokens, STATE), 1) // HEAD_DIM

    def conv(i, c, tap_ref):
        window = pad_ref[i, pl.ds(pl.multiple_of(c * tokens, tokens), tokens + 2 * margin)]
        total = window[margin - half : margin - half + tokens] * tap_ref[0:1]
        for j in range(1, taps):
            first = margin - half + j
            total = total + window[first : first + tokens] * tap_ref[j : j + 1]
        return silu(total)

    def spread_heads(cols, g):
        wide = jnp.broadcast_to(cols[g * per_group], (tokens, STATE))
        for k in range(1, per_group):
            wide = jnp.where(
                lane == k, jnp.broadcast_to(cols[g * per_group + k], (tokens, STATE)), wide
            )
        return wide

    def forward(c, _):
        at = pl.ds(pl.multiple_of(c * tokens, tokens), tokens)
        signal = conv(0, c, tx_ref)
        write = conv(1, c, tb_ref).astype(bf16)
        read = conv(2, c, tc_ref).astype(bf16)
        sig_ref[at] = signal
        wr_ref[at] = write
        rd_ref[at] = read
        raw = in_ref[c, 3 * tokens : 3 * tokens + STEP_ROWS, :tokens].astype(f32)
        step = jnp.maximum(raw, 0.0) + jnp.log1p(jnp.exp(-jnp.abs(raw)))
        drop = step * rates
        incl = jnp.dot(drop, upto, precision=highest, preferred_element_type=f32)
        excl = incl - drop
        stacked = jnp.concatenate(
            [incl, excl, step, jnp.zeros((tokens - 3 * STEP_ROWS, tokens), f32)], axis=0
        )
        cols = stacked.T
        col_ref[at] = cols

        def col(kind, row):
            return cols[:, kind * STEP_ROWS + row : kind * STEP_ROWS + row + 1]

        signal_b = signal.astype(bf16)
        reach = [col(0, 2 * h) for h in range(heads)]
        last = [incl[2 * h : 2 * h + 1, tokens - 1 : tokens] for h in range(heads)]
        scale = [col(2, 2 * h) * jnp.exp(reach[h] - last[h]) for h in range(heads)]
        fade = [jnp.exp(-reach[h]) for h in range(heads)]
        keep = [jnp.broadcast_to(jnp.exp(-last[h]), (tokens, 1)) for h in range(heads)]
        for g in range(groups):
            lanes = slice(g * STATE, (g + 1) * STATE)
            read_g = read[:, lanes]
            write_g = write[:, lanes]
            match = nt_dot(read_g, write_g)
            pieces = []
            for h in range(g * per_group, (g + 1) * per_group):
                f, b = 2 * h, 2 * h + 1
                gap = jnp.where(
                    lower, incl[f : f + 1] - reach[h], col(1, b) - excl[b : b + 1]
                )
                weight = jnp.exp(gap) * (
                    jnp.where(lower, step[f : f + 1], 0.0) + jnp.where(upper, step[b : b + 1], 0.0)
                )
                pieces.append(
                    jnp.dot(
                        (match * weight).astype(bf16),
                        signal_b[:, h * HEAD_DIM : (h + 1) * HEAD_DIM],
                        preferred_element_type=f32,
                    )
                )
            state = fwd_ref[g]
            carried = jnp.dot(read_g, state.astype(bf16), preferred_element_type=f32)
            acc_ref[at, lanes] = jnp.concatenate(pieces, axis=1) + carried * spread_heads(fade, g)
            fresh = tn_dot(write_g, (signal[:, lanes] * spread_heads(scale, g)).astype(bf16))
            fwd_ref[g] = state * spread_heads(keep, g) + fresh
        return 0

    lax.fori_loop(0, blocks, forward, 0)

    def backward(i, _):
        c = blocks - 1 - i
        at = pl.ds(pl.multiple_of(c * tokens, tokens), tokens)
        cols = col_ref[at]
        signal = sig_ref[at]
        write = wr_ref[at]
        read = rd_ref[at]

        def col(kind, row):
            return cols[:, kind * STEP_ROWS + row : kind * STEP_ROWS + row + 1]

        ahead = [col(1, 2 * h + 1) for h in range(heads)]
        whole = [col(0, 2 * h + 1)[tokens - 1 : tokens] for h in range(heads)]
        scale = [col(2, 2 * h + 1) * jnp.exp(-ahead[h]) for h in range(heads)]
        fade = [jnp.exp(ahead[h] - whole[h]) for h in range(heads)]
        keep = [jnp.broadcast_to(jnp.exp(-whole[h]), (tokens, 1)) for h in range(heads)]
        for g in range(groups):
            lanes = slice(g * STATE, (g + 1) * STATE)
            state = bwd_ref[g]
            carried = jnp.dot(read[:, lanes], state.astype(bf16), preferred_element_type=f32)
            o_ref[c, :, lanes] = (acc_ref[at, lanes] + carried * spread_heads(fade, g)).astype(bf16)
            fresh = tn_dot(write[:, lanes], (signal[:, lanes] * spread_heads(scale, g)).astype(bf16))
            bwd_ref[g] = state * spread_heads(keep, g) + fresh
        return 0

    lax.fori_loop(0, blocks, backward, 0)


def mixer(arrived, conv_x, conv_b, conv_c, decay_rate):
    blocks, rows, width = arrived.shape
    tokens = (rows - STEP_ROWS) // 3
    length = blocks * tokens
    groups = width // STATE
    rates = decay_rate.T.reshape(-1, 1)
    rates = jnp.pad(rates, ((0, STEP_ROWS - rates.shape[0]), (0, 0)))
    return pl.pallas_call(
        mixer_body,
        out_shape=jax.ShapeDtypeStruct((blocks, tokens, width), bf16),
        scratch_shapes=[
            pltpu.VMEM((3, length + 16, width), f32),
            pltpu.VMEM((length, width), f32),
            pltpu.VMEM((length, width), bf16),
            pltpu.VMEM((length, width), bf16),
            pltpu.VMEM((length, tokens), f32),
            pltpu.VMEM((length, width), f32),
            pltpu.VMEM((groups, STATE, STATE), f32),
            pltpu.VMEM((groups, STATE, STATE), f32),
        ],
        compiler_params=pltpu.CompilerParams(vmem_limit_bytes=32 * 1024 * 1024),
        name="mixer",
    )(arrived, conv_x, conv_b, conv_c, rates)


def project_body(place_ref, mix_ref, gate_ref, gain_ref, res_ref, fgain_ref, *rest):
    *w_refs, stream_ref, rows_ref, mixed_ref = rest
    n = pl.program_id(0)
    parts, tokens, part_width = mix_ref.shape
    model = gate_ref.shape[1]
    span = model // NORM_GROUPS
    each = span // part_width
    seg = mixed_ref.shape[2]
    unit = min(seg, span)
    block = w_refs[0].shape[1]

    @pl.when(n == 0)
    def _():
        for q in range(NORM_GROUPS):
            piece = jnp.concatenate([mix_ref[q * each + i] for i in range(each)], axis=1)
            cols = slice(q * span, (q + 1) * span)
            value = piece.astype(f32) * silu(gate_ref[:, cols].astype(f32))
            norm = lax.rsqrt(jnp.mean(value * value, axis=-1, keepdims=True) + epsilon)
            value = (value * norm * gain_ref[:, cols]).astype(bf16)
            for u in range(0, span, unit):
                at = q * span + u
                mixed_ref[at // seg, :, at % seg : at % seg + unit] = value[:, u : u + unit]

    total = res_ref[...].astype(f32)
    for m in range(len(w_refs)):
        total = total + jnp.dot(
            mixed_ref[place_ref[0] ^ m], w_refs[m][...], preferred_element_type=f32
        )
    stream_ref[:, pl.ds(pl.multiple_of(n * block, block), block)] = total

    @pl.when(n == pl.num_programs(0) - 1)
    def _():
        stream = stream_ref[...]
        norm = lax.rsqrt(jnp.mean(stream * stream, axis=-1, keepdims=True) + epsilon)
        rows = (stream * norm * fgain_ref[...]).astype(bf16)
        rows_ref[...] = rows


def project(place, mix, gate, gain, weights, residual, fgain):
    tokens, model = gate.shape
    block = model // 4
    seg = weights[0].shape[0]

    def whole(shape):
        return pl.BlockSpec(shape, lambda n: (0,) * len(shape))

    return pl.pallas_call(
        project_body,
        grid=(model // block,),
        in_specs=[
            pl.BlockSpec(memory_space=pltpu.SMEM),
            whole(mix.shape),
            whole(gate.shape),
            whole((1, model)),
            pl.BlockSpec((tokens, block), lambda n: (0, n)),
            whole((1, model)),
        ]
        + [pl.BlockSpec((seg, block), lambda n: (0, n))] * len(weights),
        out_specs=[whole((tokens, model)), whole((tokens, model))],
        out_shape=[
            jax.ShapeDtypeStruct((tokens, model), f32),
            jax.ShapeDtypeStruct((tokens, model), bf16),
        ],
        scratch_shapes=[pltpu.VMEM((model // seg, tokens, seg), bf16)],
        compiler_params=pltpu.CompilerParams(vmem_limit_bytes=48 * 1024 * 1024),
        name="project",
    )(place, mix, gate, gain.reshape(1, -1), residual, fgain.reshape(1, -1), *weights)


def slot_maps(routes, weights, first, experts, capacity):
    tokens = routes.shape[0]
    hits = routes.T[:, None, :] == (first + lax.iota(jnp.int32, experts))[None, :, None]
    mask = jnp.any(hits, axis=0)
    share = jnp.sum(jnp.where(hits, weights.T[:, None, :], 0.0), axis=0)
    earlier = (lax.iota(jnp.int32, tokens)[:, None] < lax.iota(jnp.int32, tokens)[None, :]).astype(
        bf16
    )
    rank = jnp.dot(mask.astype(bf16), earlier, preferred_element_type=f32).astype(jnp.int32)
    rank = jnp.where(mask, rank, capacity)
    chosen = rank[:, None, :] == lax.iota(jnp.int32, capacity)[None, :, None]
    select = chosen.astype(bf16).reshape(experts * capacity, tokens)
    share_top = share.astype(bf16)
    share_rest = (share - share_top.astype(f32)).astype(bf16)
    shares = jnp.stack([share_top, share_rest])
    merge = jnp.where(chosen[None], shares[:, :, None, :], jnp.zeros((), bf16)).reshape(
        2, experts * capacity, tokens
    )
    return select, merge


def weighted_sum(merge, answers):
    both = jnp.einsum("ast,sd->atd", merge, answers, preferred_element_type=f32)
    return both[0] + both[1]


def expert_body(rows_ref, gate_ref, up_ref, down_ref, o_ref, acc_ref):
    j = pl.program_id(0)
    rows = rows_ref[...]
    gate_value = jnp.minimum(
        jnp.dot(rows, gate_ref[...], preferred_element_type=f32), clamp_limit
    )
    up_value = jnp.clip(
        jnp.dot(rows, up_ref[...], preferred_element_type=f32), -clamp_limit, clamp_limit
    )
    squash = 1.0 / (1.0 + jnp.exp(-sigmoid_slope * gate_value))
    active = ((up_value + 1.0) * gate_value * squash).astype(bf16)
    part = jnp.dot(active, down_ref[...], preferred_element_type=f32)
    last = pl.num_programs(0) - 1

    @pl.when(j == 0)
    def _():
        acc_ref[...] = part

    @pl.when((j > 0) & (j < last))
    def _():
        acc_ref[...] += part

    @pl.when(j == last)
    def _():
        o_ref[...] = (acc_ref[...] + part).astype(bf16)


def expert_apply(rows, gate_mat, up_mat, down_mat):
    count, model = rows.shape
    hidden = gate_mat.shape[1]
    block = hidden // 4
    wide = pl.BlockSpec((count, model), lambda j: (0, 0))
    into = pl.BlockSpec((model, block), lambda j: (0, j))
    return pl.pallas_call(
        expert_body,
        grid=(hidden // block,),
        in_specs=[wide, into, into, pl.BlockSpec((block, model), lambda j: (j, 0))],
        out_specs=wide,
        out_shape=jax.ShapeDtypeStruct((count, model), bf16),
        scratch_shapes=[pltpu.VMEM((count, model), f32)],
        compiler_params=pltpu.CompilerParams(vmem_limit_bytes=48 * 1024 * 1024),
        cost_estimate=pl.CostEstimate(
            flops=6 * count * model * hidden,
            bytes_accessed=2 * (3 * model * hidden + 2 * count * model),
            transcendentals=count * hidden,
        ),
        name="expert",
    )(rows, gate_mat, up_mat, down_mat)


def per_device(
    residual_in,
    ssm_input,
    state_b,
    state_c,
    step_raw,
    gate_input,
    conv_x,
    conv_b,
    conv_c,
    decay_rate,
    mix_gain,
    out_weight,
    ffn_gain,
    routing,
    route_weight,
    gate_w,
    up_w,
    down_w,
):
    sp_axes = ("half", "rest")
    group_axes = ("rest", "dp")
    sp_count = lax.axis_size(sp_axes)
    dp_count = lax.axis_size("dp")
    group = lax.axis_size(group_axes)
    experts_all = sp_count * dp_count
    token_count = residual_in.shape[1]
    model_width = residual_in.shape[2]
    top_count = routing.shape[2]
    capacity = 2 * token_count * top_count // experts_all
    swap = [(0, 1), (1, 0)]

    def spread(pieces, bit):
        steps_of = [(i, i ^ bit) for i in range(dp_count)]
        fresh = {m ^ bit: lax.ppermute(piece, "dp", steps_of) for m, piece in pieces.items()}
        return {**pieces, **fresh}

    pieces = {0: out_weight}
    bit = dp_count // 2
    while bit > 1:
        pieces = spread(pieces, bit)
        bit //= 2

    steps = step_raw[0].T.reshape(sp_count, -1, token_count)
    steps = jnp.pad(steps, ((0, 0), (0, STEP_ROWS - steps.shape[1]), (0, 0)))
    packed = pack_inputs(ssm_input[0], state_b[0], state_c[0], steps, sp_count)
    arrived_mix = lax.all_to_all(packed, sp_axes, split_axis=0, concat_axis=0, tiled=True)
    mixed_heads = mixer(arrived_mix, conv_x, conv_b, conv_c, decay_rate)
    mixed_heads, pieces, routes, weights = lax.optimization_barrier(
        (mixed_heads, pieces, routing[0], route_weight[0])
    )
    mixed_tokens = lax.all_to_all(mixed_heads, sp_axes, split_axis=0, concat_axis=0, tiled=True)
    other_routes = lax.ppermute(routes, "half", swap)
    other_weight = lax.ppermute(weights, "half", swap)
    if bit:
        pieces = spread(pieces, bit)
    mixed_tokens, other_routes, other_weight = lax.optimization_barrier(
        (mixed_tokens, other_routes, other_weight)
    )

    first = lax.axis_index("half") * group
    select, merge = slot_maps(routing[0], route_weight[0], first, group, capacity)
    other_select, other_merge = slot_maps(other_routes, other_weight, first, group, capacity)

    stream, rows = project(
        lax.axis_index("dp").reshape(1),
        mixed_tokens,
        gate_input[0],
        mix_gain,
        [pieces[m] for m in range(dp_count)],
        residual_in[0],
        ffn_gain,
    )

    def exchange(slots):
        return lax.all_to_all(
            slots.reshape(group, capacity, model_width),
            group_axes,
            split_axis=0,
            concat_axis=0,
            tiled=True,
        ).reshape(group * capacity, model_width)

    other_rows = lax.ppermute(rows, "half", swap)
    arrived = exchange(jnp.dot(select, rows, preferred_element_type=f32).astype(bf16))
    other_rows, arrived = lax.optimization_barrier((other_rows, arrived))
    other_arrived = exchange(
        jnp.dot(other_select, other_rows, preferred_element_type=f32).astype(bf16)
    )
    served = expert_apply(arrived, gate_w[0], up_w[0], down_w[0])
    other_served = expert_apply(other_arrived, gate_w[0], up_w[0], down_w[0])
    other_answers = exchange(other_served)
    other_sum = weighted_sum(other_merge, other_answers).astype(bf16)
    served, other_sum = lax.optimization_barrier((served, other_sum))
    from_other = lax.ppermute(other_sum, "half", swap)
    answers = exchange(served)
    return (stream + weighted_sum(merge, answers) + from_other.astype(f32)).astype(bf16)[None]


def solution(mesh):
    devices = mesh.devices
    halves = jax.sharding.Mesh(
        devices.reshape(2, devices.shape[0] // 2, devices.shape[1]), ("half", "rest", "dp")
    )
    return jax.shard_map(
        per_device,
        mesh=halves,
        in_specs=(
            P("dp", ("half", "rest"), None),
            P("dp", ("half", "rest"), None),
            P("dp", ("half", "rest"), None),
            P("dp", ("half", "rest"), None),
            P("dp", ("half", "rest"), None),
            P("dp", ("half", "rest"), None),
            P(None, ("half", "rest")),
            P(None, ("half", "rest")),
            P(None, ("half", "rest")),
            P(None, ("half", "rest")),
            P(),
            P("dp", None),
            P(),
            P("dp", ("half", "rest"), None),
            P("dp", ("half", "rest"), None),
            P(("half", "rest", "dp"), None, None),
            P(("half", "rest", "dp"), None, None),
            P(("half", "rest", "dp"), None, None),
        ),
        out_specs=P("dp", ("half", "rest"), None),
        check_vma=False,
    )
```
